32 devices in a mesh: sp: 16 (over z, y, x), tp: 2 (over core).
Axes of the slice: x: 2, y: 2, z: 4, core: 2. Of those that a mesh axis runs over, the one named last changes fastest.
Arguments:
- residual: bfloat16 [2048, 2048], P(('sp', 'tp')), may hold values from -6 to 6
- conv_input: bfloat16 [2048, 1024], P('sp', 'tp'), may hold values from -6 to 6
- input_gate: bfloat16 [2048, 1024], P('sp', 'tp'), may hold values from -6 to 6
- output_gate: bfloat16 [2048, 1024], P('sp', 'tp'), may hold values from -6 to 6
- conv_taps: bfloat16 [3, 1024], P(None, 'tp'), may hold values from -3.5 to 3.5
- out_proj: bfloat16 [1024, 2048], P('tp'), may hold values from -0.1875 to 0.1875
- norm_gain: float32 [2048], replicated, may hold values from 0.1 to 1.9
- routes: int32 [2048, 2], P(('sp', 'tp')), may hold values from 0 to 15, all different within a row; in each aligned block of 64 rows (0 to 63, 64 to 127, ...) at most 16 rows name the same one
- route_weight: float32 [2048, 2], P(('sp', 'tp')), may hold values from 0.1 to 1
- gate_proj: bfloat16 [16, 2048, 3584], P('sp', None, 'tp'), may hold values from -0.125 to 0.125
- up_proj: bfloat16 [16, 2048, 3584], P('sp', None, 'tp'), may hold values from -0.125 to 0.125
- down_proj: bfloat16 [16, 3584, 2048], P('sp', 'tp'), may hold values from -0.09375 to 0.09375
Outputs:
- layer_out: bfloat16 [2048, 2048], P(('sp', 'tp'))
The draws below stay inside these ranges and needn't reach their ends.
Inputs may be any that keep to these rules, and one draw needn't show every extreme that they name: `routes`: A token's 2 experts differ. Among the 64 tokens of one device, in the aligned blocks of the tokens' order, no expert is named more than 16 times, a bound that some block reaches in some device.
All inputs are finite; a program needn't handle non-finite values.
Results may differ from the reference program's by a relative error of at most 0.0054.
Values may be sent and summed in bfloat16 or wider, within the bound.
A program may use at most 128 MiB of HBM per device.

```python
import math
import jax
import jax.numpy as jnp
import numpy as np
from jax import lax

D = 2048
CW = 1024
FF = 3584
KSIZE = 3
TOPK = 2
TOK_SH = 64
TOKENS = 2048
EXPERTS = 16
CAP = 16
N_SP = 16
N_TP = 2


def level_of(key, dims, cuts, smallest, largest):
    gain, own = 1.0, jax.random.fold_in(key, 6)
    for position, blocks in cuts:
        steps = jnp.exp(jax.random.uniform(jax.random.fold_in(own, position), (blocks,), jnp.float32, smallest / len(cuts), largest / len(cuts)))
        gain = gain * jnp.repeat(steps, dims[position] // blocks).reshape([-1 if axis == position else 1 for axis in range(len(dims))])
    return gain


def routed_block(key, own, number, rows, count, top, limit, lean):
    order = jax.random.permutation(key, count)
    packed, usual = load_shares(count, rows * top, limit, lean, True), load_shares(count, rows * top, limit, lean, False)
    places = jnp.arange(count)

    def named(lengths, rotation):
        used = int((lengths > 0).sum())
        fixed = max(1, used // 4)
        passed = fixed + (places - fixed + rotation * (used - fixed)) % max(1, count - fixed)
        return jnp.zeros((count,), jnp.int32).at[order[jnp.where(places < fixed, places, passed)]].set(jnp.asarray(lengths, jnp.int32))

    lengths = jnp.where(number % 4 == 0, named(packed, number // 4), named(usual, number - number // 4 - 1))
    mixed = jax.random.permutation(jax.random.fold_in(own, 3), count)
    donor, receiver = mixed[0:count // 2 * 2:2], mixed[1:count // 2 * 2:2]
    margin = jnp.minimum(lengths[donor] - 1, limit - lengths[receiver]) // 2
    margin = jnp.where((donor == order[0]) | (receiver == order[0]) | (lengths[receiver] == 0), 0, jnp.maximum(margin, 0))
    passed = jax.random.randint(jax.random.fold_in(own, 4), (count // 2,), 0, 1 << 20) % (margin + 1)
    lengths = lengths.at[donor].add(-passed).at[receiver].add(passed)
    items = jnp.searchsorted(jnp.cumsum(lengths), jnp.arange(rows * top), side="right").astype(jnp.int32)
    table = items.reshape(top, rows).T
    table = table[jax.random.permutation(jax.random.fold_in(own, 1), rows)]
    rotation = jax.random.randint(jax.random.fold_in(own, 2), (rows, 1), 0, top)
    return jnp.take_along_axis(table, (jnp.arange(top)[None, :] + rotation) % top, axis=1)


def load_shares(amount, total, limit, lean, full):
    portions = [(1 << 20) // math.isqrt(rank ** lean) + 1 for rank in range(1, amount + 1)]
    largest = limit if full else min(limit, max(-(-total // amount), total * portions[0] // sum(portions)))
    least = 1 if total - largest >= amount - 1 else 0
    given, spare = [largest] + [least] * (amount - 1), total - largest - least * (amount - 1)
    while spare > 0:
        movable = [i for i in range(1, amount) if given[i] < largest] or [i for i in range(1, amount) if given[i] < limit]
        pool, budget = sum([portions[i] for i in movable]), spare
        for i in movable:
            addition = min(limit - given[i], max(1, budget * portions[i] // pool), spare)
            given[i] = given[i] + addition
            spare = spare - addition
    return np.array(given)


def centred(stream_key, extent, scale, limit, pieces=(), kind=jnp.bfloat16):
    entries = scale * jax.random.normal(stream_key, extent, jnp.float32)
    if pieces:
        entries = entries * level_of(stream_key, extent, pieces, -0.22, 0.18)
    return jnp.clip(entries, -limit, limit).astype(kind)


def setup_inputs(seed: int = 0) -> dict:
    streams_of = jax.random.split(jax.random.key(seed), 13)
    residual = centred(streams_of[0], (TOKENS, D), 1.0, 6.0, ((0, 32),))
    conv_input = centred(streams_of[1], (TOKENS, CW), 1.0, 6.0, ((0, 16), (1, 2)))
    input_gate = centred(streams_of[2], (TOKENS, CW), 1.0, 6.0, ((0, 16), (1, 2)))
    output_gate = centred(streams_of[3], (TOKENS, CW), 1.0, 6.0, ((0, 16), (1, 2)))
    conv_taps = centred(streams_of[4], (KSIZE, CW), KSIZE ** -0.5, 3.5, ((1, 2),))
    out_proj = centred(streams_of[5], (CW, D), CW ** -0.5, 0.1875, ((0, 2),))
    norm_gain = jnp.clip(1.0 + 0.18 * jax.random.normal(streams_of[6], (D,), jnp.float32), 0.1, 1.9)
    routes_keys = jax.random.split(jax.random.fold_in(streams_of[7], 1), TOKENS // TOK_SH)
    routes_turns = jax.random.permutation(jax.random.fold_in(streams_of[7], 3), TOKENS // TOK_SH)
    routes = jax.vmap(lambda own, number: routed_block(jax.random.fold_in(streams_of[7], 2), own, number, TOK_SH, EXPERTS, TOPK, CAP, 2))(routes_keys, routes_turns).reshape((TOKENS, TOPK))
    route_weight = jnp.clip(0.1 + 0.9 * jax.random.uniform(streams_of[8], (TOKENS, TOPK), jnp.float32) ** level_of(streams_of[8], (TOKENS, TOPK), ((0, 32),), -0.2, 0.2), 0.1, 1.0)
    gate_proj = centred(streams_of[9], (EXPERTS, D, FF), D ** -0.5, 0.125, ((0, 16), (2, 2)))
    up_proj = centred(streams_of[10], (EXPERTS, D, FF), D ** -0.5, 0.125, ((0, 16), (2, 2)))
    down_proj = centred(streams_of[11], (EXPERTS, FF, D), FF ** -0.5, 0.09375, ((0, 16), (1, 2)))
    return {"residual": residual, "conv_input": conv_input, "input_gate": input_gate, "output_gate": output_gate, "conv_taps": conv_taps, "out_proj": out_proj, "norm_gain": norm_gain, "routes": routes, "route_weight": route_weight, "gate_proj": gate_proj, "up_proj": up_proj, "down_proj": down_proj}


def reference(residual, conv_input, input_gate, output_gate, conv_taps, out_proj, norm_gain, routes, route_weight, gate_proj, up_proj, down_proj):
    tap_count = conv_taps.shape[0]
    length = conv_input.shape[0]
    mixed = input_gate.astype(jnp.float32) * conv_input.astype(jnp.float32)
    padded = jnp.pad(mixed, ((tap_count - 1, 0), (0, 0)))
    convolved = jnp.zeros_like(mixed)
    for tap_index in range(tap_count):
        convolved = convolved + conv_taps[tap_index].astype(jnp.float32)[None, :] * padded[tap_index:tap_index + length]
    gated_rows = (output_gate.astype(jnp.float32) * convolved).astype(jnp.bfloat16)
    stream = residual.astype(jnp.float32) + jnp.dot(gated_rows, out_proj, preferred_element_type=jnp.float32)
    inverse_rms = lax.rsqrt(lax.optimization_barrier(jnp.mean(stream * stream, axis=-1, keepdims=True)) + 1e-06)
    normed = (stream * inverse_rms * norm_gain.astype(jnp.float32)[None, :]).astype(jnp.bfloat16)
    blocks = N_SP * N_TP
    tok_rows = TOKENS // blocks
    per_block = tok_rows * TOPK
    flat_routes = routes.reshape(blocks, per_block)
    onehot = (flat_routes[:, :, None] == jnp.arange(EXPERTS, dtype=jnp.int32)[None, None, :]).astype(jnp.int32)
    counts = jnp.cumsum(onehot, axis=1)
    slot_ids = lax.optimization_barrier(jnp.sum(onehot * (counts - 1), axis=2)).astype(jnp.int32)
    token_ids = (jnp.arange(blocks * per_block, dtype=jnp.int32) // TOPK).reshape(blocks, per_block)
    block_ids = jnp.broadcast_to(jnp.arange(blocks, dtype=jnp.int32)[:, None], (blocks, per_block))
    slot_table = jnp.zeros((EXPERTS, blocks, CAP), jnp.int32).at[flat_routes, block_ids, slot_ids].set(token_ids)
    weight_table = jnp.zeros((EXPERTS, blocks, CAP), jnp.float32).at[flat_routes, block_ids, slot_ids].set(route_weight.astype(jnp.float32).reshape(blocks, per_block))
    half_width = FF // N_TP

    def expert_step(running, inputs):
        ids_here, weights_here, gate_part, up_part, down_part = inputs
        flat_ids = ids_here.reshape(-1)
        flat_rows = normed[flat_ids]
        summed = jnp.zeros((flat_rows.shape[0], flat_rows.shape[1]), jnp.float32)
        for half_index in range(N_TP):
            lower = half_index * half_width
            upper = lower + half_width
            gate_val = jnp.dot(flat_rows, gate_part[:, lower:upper], preferred_element_type=jnp.float32)
            up_val = jnp.dot(flat_rows, up_part[:, lower:upper], preferred_element_type=jnp.float32)
            active = (jax.nn.silu(gate_val) * up_val).astype(jnp.bfloat16)
            partial_value = jnp.dot(active, down_part[lower:upper], preferred_element_type=jnp.float32).astype(jnp.bfloat16)
            partial_value = lax.optimization_barrier(partial_value)
            summed = summed + partial_value.astype(jnp.float32)
        halves = lax.optimization_barrier(summed.astype(jnp.bfloat16))
        running = running.at[flat_ids].add(weights_here.reshape(-1)[:, None] * halves.astype(jnp.float32))
        return (running, None)
    routed, _ = lax.scan(expert_step, jnp.zeros((TOKENS, D), jnp.float32), (slot_table, weight_table, gate_proj, up_proj, down_proj))
    return (stream + routed).astype(jnp.bfloat16)
```

```python
import functools

import jax
import jax.numpy as jnp
from jax import lax
from jax.experimental import pallas as pl
from jax.experimental.pallas import tpu as pltpu
from jax.sharding import PartitionSpec as P

MESH = pl.DeviceIdType.MESH
F32 = jnp.float32
BF16 = jnp.bfloat16
RIM = 16


IN_TILE = 1792
OUT_TILE = 1024


def tile_of(size, most):
    for tile in range(most, 127, -128):
        if size % tile == 0:
            return tile
    return size


def dot(a, b):
    return jnp.dot(a, b, preferred_element_type=F32)


def kernel(
    peers,
    groups,
    rows,
    residual_hbm,
    conv_input_hbm,
    input_gate_hbm,
    output_gate_hbm,
    taps_hbm,
    gain_hbm,
    routes_hbm,
    weights_hbm,
    out_proj_hbm,
    gate_hbm,
    up_hbm,
    down_hbm,
    out,
    residual,
    conv_input,
    input_gate,
    output_gate,
    taps,
    gain,
    routes,
    weights,
    out_proj,
    gate,
    up,
    down,
    rim,
    ext,
    chosen,
    proj,
    proj_in,
    raw,
    raw_in,
    chosen_in,
    outgoing,
    recv,
    active,
    part,
    part_in,
    ret,
    spread,
    load_sem,
    rim_send,
    rim_recv,
    proj_send,
    proj_recv,
    raw_send,
    raw_recv,
    chosen_send,
    chosen_recv,
    out_send,
    out_recv,
    fwd_send,
    fwd_recv,
    part_send,
    part_recv,
    ret_send,
    ret_recv,
):
    me = lax.axis_index("sp")
    core = lax.axis_index("tp")
    other = 1 - core
    length, channels = conv_input.shape
    tokens, width = residual.shape
    hidden = gate.shape[1]
    tap_count = taps.shape[0]
    per_group = peers // groups

    barrier = pltpu.get_barrier_semaphore()

    @pl.loop(1, peers)
    def _(k):
        pl.semaphore_signal(
            barrier, inc=1, device_id=(lax.rem(me + k, peers), core), device_id_type=MESH
        )

    pl.semaphore_signal(barrier, inc=1, device_id=(me, other), device_id_type=MESH)

    loads = []
    for i, (src, dst) in enumerate(
        (
            (routes_hbm, routes),
            (weights_hbm, weights),
            (conv_input_hbm, conv_input),
            (input_gate_hbm, input_gate),
            (output_gate_hbm, output_gate),
            (taps_hbm, taps),
            (out_proj_hbm, out_proj),
            (residual_hbm, residual),
            (gain_hbm, gain),
            (gate_hbm.at[0], gate),
            (up_hbm.at[0], up),
            (down_hbm.at[0], down),
        )
    ):
        load = pltpu.make_async_copy(src, dst, load_sem.at[i])
        load.start()
        loads.append(load)

    loads[0].wait()
    loads[1].wait()
    tops = routes.shape[0]
    ids = lax.broadcasted_iota(jnp.int32, (peers, tokens), 0)
    hots = [(routes[k : k + 1, :] == ids).astype(F32) for k in range(tops)]
    total = functools.reduce(jnp.add, hots)
    earlier = (
        lax.broadcasted_iota(jnp.int32, (tokens, tokens), 0)
        < lax.broadcasted_iota(jnp.int32, (tokens, tokens), 1)
    ).astype(BF16)
    counts = dot(total.astype(BF16), earlier)
    lines = lax.broadcasted_iota(jnp.int32, (peers * rows, tokens), 0)
    select = jnp.zeros((peers * rows, tokens), F32)
    weigh = jnp.zeros((peers * rows, tokens), F32)
    for k in range(tops):
        slot = jnp.sum(counts * hots[k], axis=0, keepdims=True).astype(jnp.int32)
        hit = lines == routes[k : k + 1, :] * rows + slot
        select = jnp.where(hit, 1.0, select)
        weigh = jnp.where(hit, weights[k : k + 1, :], weigh)
    chosen[...] = select.astype(BF16)
    half = per_group * rows
    for g in range(groups):
        rest = weigh[g * half : (g + 1) * half].T
        pieces = []
        for _ in range(3):
            piece = rest.astype(BF16).astype(F32)
            pieces.append(piece)
            rest = rest - piece
        spread[g] = jnp.concatenate(pieces, axis=1).astype(BF16)

    for i in range(2, 6):
        loads[i].wait()
    ext[pl.ds(RIM, length)] = input_gate[...].astype(F32) * conv_input[...].astype(F32)

    def gate_rows(lane):
        convolved = jnp.zeros((tokens, channels), F32)
        for j in range(tap_count):
            convolved = convolved + taps[j : j + 1, :].astype(F32) * ext[
                pl.ds(RIM - tap_count + 1 + j + lane * tokens, tokens)
            ]
        opened = output_gate[pl.ds(lane * tokens, tokens)].astype(F32)
        return (opened * convolved).astype(BF16)

    late = gate_rows(1)
    loads[6].wait()
    proj[1] = dot(late, out_proj[...])

    pl.semaphore_wait(barrier, peers)

    def rim_copy(which, target):
        src = (conv_input, input_gate)[which]
        return pltpu.make_async_remote_copy(
            src_ref=src.at[pl.ds(length - RIM, RIM)],
            dst_ref=rim.at[which],
            send_sem=rim_send.at[which],
            recv_sem=rim_recv.at[which],
            device_id=(target, core),
            device_id_type=MESH,
        )

    @pl.when(me < peers - 1)
    def _():
        for which in range(2):
            rim_copy(which, me + 1).start()

    proj_copy = pltpu.make_async_remote_copy(
        src_ref=proj.at[other],
        dst_ref=proj_in,
        send_sem=proj_send,
        recv_sem=proj_recv,
        device_id=(me, other),
        device_id_type=MESH,
    )

    @pl.when(core == 0)
    def _():
        proj_copy.start()

    @pl.when(me == 0)
    def _():
        ext[pl.ds(0, RIM)] = jnp.zeros((RIM, channels), F32)

    @pl.when(me > 0)
    def _():
        for which in range(2):
            rim_copy(which, me).wait_recv()
        ext[pl.ds(0, RIM)] = rim[1].astype(F32) * rim[0].astype(F32)

    proj[0] = dot(gate_rows(0), out_proj[...])

    @pl.when(core == 1)
    def _():
        proj_copy.start()

    loads[7].wait()
    loads[8].wait()
    proj_copy.wait_recv()
    stream = residual[...].astype(F32) + (proj[core] + proj_in[...])
    inverse_rms = lax.rsqrt(jnp.mean(stream * stream, axis=-1, keepdims=True) + 1e-06)
    normed = (stream * inverse_rms * gain[...]).astype(BF16)
    raw[...] = normed

    mine = me // per_group
    span_rows = per_group * rows
    if groups == 4:
        near = mine // 2 * 2
        far = lax.rem(near + 2, 4)
        side = mine - near
        beside, across, mirror = near + 1 - side, far + side, far + 1 - side
        middle = lax.rem(mine // 2 + side, 2)
        order = [
            mine,
            beside + middle * (mirror - beside),
            mirror + middle * (beside - mirror),
            across,
        ]
        back = [mine, beside, mirror, across]
        sends = [mine, beside]
        distant = [mirror, across]
        partner = me + middle * (mirror - mine) * per_group
    else:
        order = back = sends = [lax.rem(mine + step, groups) for step in range(groups)]
        distant = []
        middle, partner = 0, me
    column_half = width // 2

    def raw_copy(part_of):
        cols = pl.ds(part_of * column_half, column_half)
        return pltpu.make_async_remote_copy(
            src_ref=raw.at[:, cols],
            dst_ref=raw_in.at[:, cols],
            send_sem=raw_send.at[part_of],
            recv_sem=raw_recv.at[part_of],
            device_id=(partner, core),
            device_id_type=MESH,
        )

    def chosen_copy():
        return pltpu.make_async_remote_copy(
            src_ref=chosen.at[pl.ds(pl.multiple_of(far * span_rows, span_rows), 2 * span_rows)],
            dst_ref=chosen_in,
            send_sem=chosen_send,
            recv_sem=chosen_recv,
            device_id=(partner, core),
            device_id_type=MESH,
        )

    if groups == 4:

        @pl.when(middle == 1)
        def _():
            chosen_copy().start()
            for part_of in range(2):
                raw_copy(part_of).start()

    def out_copy(slot, src, target):
        return pltpu.make_async_remote_copy(
            src_ref=outgoing.at[slot],
            dst_ref=recv.at[core, src],
            send_sem=out_send.at[slot],
            recv_sem=out_recv.at[src],
            device_id=(target, core),
            device_id_type=MESH,
        )

    def send_plane(plane):
        picked = chosen[pl.ds(pl.multiple_of(plane * span_rows, span_rows), span_rows)]
        slots = dot(picked, normed).astype(BF16).reshape(per_group, rows, width)
        outgoing[pl.ds(plane * per_group, per_group)] = slots

        @pl.loop(0, per_group)
        def _(i):
            target = plane * per_group + lax.rem(me + i, per_group)

            @pl.when(target != me)
            def _():
                out_copy(target, me, target).start()

    for plane in sends:
        send_plane(plane)
    recv[core, me] = outgoing[me]
    if groups == 4:

        @pl.when(middle == 0)
        def _():
            for plane in distant:
                send_plane(plane)

    proj_copy.wait_send()
    proj[core] = stream

    def fwd_copy(src, lane):
        return pltpu.make_async_remote_copy(
            src_ref=recv.at[lane, src],
            dst_ref=recv.at[lane, src],
            send_sem=fwd_send.at[src],
            recv_sem=fwd_recv.at[src],
            device_id=(me, other),
            device_id_type=MESH,
        )

    def ret_copy(src, slot, target):
        return pltpu.make_async_remote_copy(
            src_ref=part.at[core, src],
            dst_ref=ret.at[slot],
            send_sem=ret_send.at[src],
            recv_sem=ret_recv.at[slot],
            device_id=(target, core),
            device_id_type=MESH,
        )

    in_tile = tile_of(hidden, IN_TILE)
    out_tile = tile_of(width // 2, OUT_TILE)
    count = per_group
    lot = count * rows

    def begin(step):
        first = order[step] * per_group

        @pl.loop(0, count)
        def _(i):
            src = first + lax.rem(me + i, count)

            @pl.when((src != me) & (src != partner))
            def _():
                out_copy(src, src, src).wait_recv()

            fwd_copy(src, core).start()

    def relay():
        chosen_copy().wait_recv()
        for part_of in range(2):
            raw_copy(part_of).wait_recv()
            cols = pl.ds(part_of * column_half, column_half)
            picked = dot(chosen_in[...], raw_in[:, cols]).astype(BF16)
            outgoing[pl.ds(far * per_group, 2 * per_group), :, cols] = picked.reshape(
                2 * per_group, rows, column_half
            )

            @pl.loop(0, 2 * per_group)
            def _(i):
                target = near * per_group + lax.rem(me + i, 2 * per_group)
                slot = lax.rem(target + peers // 2, peers)

                @pl.when(target != me)
                def _():
                    pltpu.make_async_remote_copy(
                        src_ref=outgoing.at[slot, :, cols],
                        dst_ref=recv.at[core, partner, :, cols],
                        send_sem=out_send.at[slot],
                        recv_sem=out_recv.at[partner],
                        device_id=(target, core),
                        device_id_type=MESH,
                    ).start()

        recv[core, partner] = outgoing[lax.rem(me + peers // 2, peers)]

    def part_copy(step, side_of):
        span = pl.ds(order[step] * per_group, count)
        part_half = pl.ds(side_of * column_half, column_half)
        return pltpu.make_async_remote_copy(
            src_ref=part.at[other, span, :, part_half],
            dst_ref=part_in.at[span, :, part_half],
            send_sem=part_send.at[step, side_of],
            recv_sem=part_recv.at[step, side_of],
            device_id=(me, other),
            device_id_type=MESH,
        )

    def raise_up(step):
        first = order[step] * per_group
        span = pl.ds(first, count)

        @pl.loop(0, count)
        def _(i):
            fwd_copy(first + lax.rem(me + i, count), other).wait_recv()

        @pl.loop(0, hidden // in_tile)
        def _(n):
            cols = pl.ds(pl.multiple_of(n * in_tile, in_tile), in_tile)
            x = recv[:, span].reshape(2 * lot, width)
            g = dot(x, gate[:, cols])
            u = dot(x, up[:, cols])
            active[:, cols] = (g * (1.0 / (1.0 + jnp.exp(-g))) * u).astype(BF16)

    def bring_down(step):
        span = pl.ds(order[step] * per_group, count)
        for side_of in range(2):
            start = side_of * column_half

            @pl.loop(0, column_half // out_tile)
            def _(n):
                cols = pl.ds(pl.multiple_of(start + n * out_tile, 128), out_tile)
                y = dot(active[...], down[:, cols]).astype(BF16)
                part[:, span, :, cols] = y.reshape(2, count, rows, out_tile)

            part_copy(step, side_of).start()

    def tail(step):
        first = order[step] * per_group
        for side_of in range(2):
            part_copy(step, side_of).wait()

        @pl.loop(0, count)
        def _(i):
            src = first + lax.rem(me + i, count)
            halves = (part[core, src].astype(F32) + part_in[src].astype(F32)).astype(BF16)
            part[core, src] = halves

            @pl.when(src != me)
            def _():
                ret_copy(src, me, src).start()

            @pl.when(src == me)
            def _():
                ret[me] = halves

    if groups == 4:

        @pl.when(middle == 1)
        def _():
            relay()

    begin(0)
    for step in range(groups):
        if step == 0:
            loads[9].wait()
            loads[10].wait()
        raise_up(step)
        if step > 0:
            tail(step - 1)
        else:
            loads[11].wait()
        if step < groups - 1:
            begin(step + 1)
        bring_down(step)
    tail(groups - 1)

    for step, plane in enumerate(back):
        first = plane * per_group

        @pl.loop(0, count)
        def _(i):
            src = first + i

            @pl.when(src != me)
            def _():
                ret_copy(src, src, src).wait_recv()

        for n in range(width // out_tile):
            cols = pl.ds(n * out_tile, out_tile)
            values = ret[pl.ds(first, count), :, cols].reshape(lot, out_tile)
            added = proj[core, :, cols] + dot(
                spread[plane], jnp.concatenate([values] * 3, axis=0)
            )
            if step < groups - 1:
                proj[core, :, cols] = added
            else:
                out[:, cols] = added.astype(BF16)

    @pl.loop(0, peers)
    def _(src):
        @pl.when((src != me) & (lax.rem(src + middle * (peers // 2), peers) != me))
        def _():
            out_copy(src, src, src).wait_send()

        @pl.when(src != me)
        def _():
            ret_copy(src, src, src).wait_send()

        fwd_copy(src, core).wait_send()

    if groups == 4:

        @pl.when(middle == 1)
        def _():
            chosen_copy().wait_send()
            for part_of in range(2):
                raw_copy(part_of).wait_send()

    @pl.when(me < peers - 1)
    def _():
        for which in range(2):
            rim_copy(which, me + 1).wait_send()


def per_device(
    residual,
    conv_input,
    input_gate,
    output_gate,
    conv_taps,
    out_proj,
    norm_gain,
    routes,
    route_weight,
    gate_proj,
    up_proj,
    down_proj,
):
    peers = lax.axis_size("sp")
    tokens, width = residual.shape
    length, channels = conv_input.shape
    hidden = gate_proj.shape[2]
    capacity = 2 * tokens * routes.shape[1] // peers
    rows = -(-capacity // 16) * 16
    groups = 4 if peers % 4 == 0 else 1
    half = peers // groups * rows
    relayed = 2 * half if groups == 4 else rows
    dma = pltpu.SemaphoreType.DMA
    vmem = pl.BlockSpec(memory_space=pltpu.VMEM)
    hbm = pl.BlockSpec(memory_space=pltpu.HBM)
    return pl.pallas_call(
        functools.partial(kernel, peers, groups, rows),
        out_shape=jax.ShapeDtypeStruct((tokens, width), BF16),
        in_specs=[hbm] * 12,
        out_specs=vmem,
        scratch_shapes=[
            pltpu.VMEM(residual.shape, BF16),
            pltpu.VMEM(conv_input.shape, BF16),
            pltpu.VMEM(input_gate.shape, BF16),
            pltpu.VMEM(output_gate.shape, BF16),
            pltpu.VMEM(conv_taps.shape, BF16),
            pltpu.VMEM((1, width), F32),
            pltpu.VMEM(routes.shape[::-1], jnp.int32),
            pltpu.VMEM(route_weight.shape[::-1], F32),
            pltpu.VMEM(out_proj.shape, BF16),
            pltpu.VMEM(gate_proj.shape[1:], BF16),
            pltpu.VMEM(up_proj.shape[1:], BF16),
            pltpu.VMEM(down_proj.shape[1:], BF16),
            pltpu.VMEM((2, RIM, channels), BF16),
            pltpu.VMEM((RIM + length, channels), F32),
            pltpu.VMEM((peers * rows, tokens), BF16),
            pltpu.VMEM((2, tokens, width), F32),
            pltpu.VMEM((tokens, width), F32),
            pltpu.VMEM((tokens, width), BF16),
            pltpu.VMEM((tokens, width), BF16),
            pltpu.VMEM((relayed, tokens), BF16),
            pltpu.VMEM((peers, rows, width), BF16),
            pltpu.VMEM((2, peers, rows, width), BF16),
            pltpu.VMEM((2 * half, hidden), BF16),
            pltpu.VMEM((2, peers, rows, width), BF16),
            pltpu.VMEM((peers, rows, width), BF16),
            pltpu.VMEM((peers, rows, width), BF16),
            pltpu.VMEM((groups, tokens, 3 * half), BF16),
            dma((12,)),
            dma((2,)),
            dma((2,)),
            dma,
            dma,
            dma((2,)),
            dma((2,)),
            dma,
            dma,
            dma((peers,)),
            dma((peers,)),
            dma((peers,)),
            dma((peers,)),
            dma((groups, 2)),
            dma((groups, 2)),
            dma((peers,)),
            dma((peers,)),
        ],
        compiler_params=pltpu.CompilerParams(
            collective_id=0, has_side_effects=True, vmem_limit_bytes=67043328
        ),
        name="mixer_experts",
    )(
        residual,
        conv_input,
        input_gate,
        output_gate,
        conv_taps,
        norm_gain.reshape(1, width),
        routes.T,
        route_weight.T,
        out_proj,
        gate_proj,
        up_proj,
        down_proj,
    )


def solution(mesh):
    return jax.shard_map(
        per_device,
        mesh=mesh,
        in_specs=(
            P(("sp", "tp"), None),
            P("sp", "tp"),
            P("sp", "tp"),
            P("sp", "tp"),
            P(None, "tp"),
            P("tp", None),
            P(),
            P(("sp", "tp"), None),
            P(("sp", "tp"), None),
            P("sp", None, "tp"),
            P("sp", None, "tp"),
            P("sp", "tp", None),
        ),
        out_specs=P(("sp", "tp"), None),
        check_vma=False,
    )
```

```python
import functools

import jax
import jax.numpy as jnp
from jax import lax
from jax.experimental import pallas as pl
from jax.experimental.pallas import tpu as pltpu
from jax.sharding import PartitionSpec as P

MESH = pl.DeviceIdType.MESH
F32 = jnp.float32
BF16 = jnp.bfloat16
RIM = 16


IN_TILE = 1792
OUT_TILE = 1024


def tile_of(size, most):
    for tile in range(most, 127, -128):
        if size % tile == 0:
            return tile
    return size


def dot(a, b):
    return jnp.dot(a, b, preferred_element_type=F32)


def kernel(
    peers,
    groups,
    rows,
    residual_hbm,
    conv_input_hbm,
    input_gate_hbm,
    output_gate_hbm,
    taps_hbm,
    gain_hbm,
    routes_hbm,
    weights_hbm,
    out_proj_hbm,
    gate_hbm,
    up_hbm,
    down_hbm,
    out_hbm,
    out,
    residual,
    conv_input,
    input_gate,
    output_gate,
    taps,
    gain,
    routes,
    weights,
    out_proj,
    gate,
    up,
    down,
    rim,
    ext,
    chosen,
    proj,
    proj_in,
    raw,
    raw_in,
    chosen_in,
    outgoing,
    recv,
    active,
    part,
    part_in,
    ret,
    spread,
    spread_in,
    gather,
    summed,
    sum_in,
    out_copy_sem,
    load_sem,
    rim_send,
    rim_recv,
    proj_send,
    proj_recv,
    raw_send,
    raw_recv,
    chosen_send,
    chosen_recv,
    out_send,
    out_recv,
    fwd_send,
    fwd_recv,
    part_send,
    part_recv,
    ret_send,
    ret_recv,
    spread_send,
    spread_recv,
    gather_recv,
    sum_send,
    sum_recv,
):
    me = lax.axis_index("sp")
    core = lax.axis_index("tp")
    other = 1 - core
    length, channels = conv_input.shape
    tokens, width = residual.shape
    hidden = gate.shape[1]
    tap_count = taps.shape[0]
    per_group = peers // groups

    barrier = pltpu.get_barrier_semaphore()


    @pl.loop(1, peers)
    def _(k):
        pl.semaphore_signal(
            barrier, inc=1, device_id=(lax.rem(me + k, peers), core), device_id_type=MESH
        )

    pl.semaphore_signal(barrier, inc=1, device_id=(me, other), device_id_type=MESH)
    mine = me // per_group

    loads = []
    for i, (src, dst) in enumerate(
        (
            (routes_hbm, routes),
            (weights_hbm, weights),
            (conv_input_hbm, conv_input),
            (input_gate_hbm, input_gate),
            (output_gate_hbm, output_gate),
            (taps_hbm, taps),
            (out_proj_hbm, out_proj),
            (residual_hbm, residual),
            (gain_hbm, gain),
            (gate_hbm.at[0], gate),
            (up_hbm.at[0], up),
            (down_hbm.at[0], down),
        )
    ):
        load = pltpu.make_async_copy(src, dst, load_sem.at[i])
        load.start()
        loads.append(load)

    loads[0].wait()
    loads[1].wait()
    tops = routes.shape[0]
    ids = lax.broadcasted_iota(jnp.int32, (peers, tokens), 0)
    hots = [(routes[k : k + 1, :] == ids).astype(F32) for k in range(tops)]
    total = functools.reduce(jnp.add, hots)
    earlier = (
        lax.broadcasted_iota(jnp.int32, (tokens, tokens), 0)
        < lax.broadcasted_iota(jnp.int32, (tokens, tokens), 1)
    ).astype(BF16)
    counts = dot(total.astype(BF16), earlier)
    lines = lax.broadcasted_iota(jnp.int32, (peers * rows, tokens), 0)
    select = jnp.zeros((peers * rows, tokens), F32)
    weigh = jnp.zeros((peers * rows, tokens), F32)
    for k in range(tops):
        slot = jnp.sum(counts * hots[k], axis=0, keepdims=True).astype(jnp.int32)
        hit = lines == routes[k : k + 1, :] * rows + slot
        select = jnp.where(hit, 1.0, select)
        weigh = jnp.where(hit, weights[k : k + 1, :], weigh)
    chosen[...] = select.astype(BF16)
    half = per_group * rows
    for g in range(groups):
        rest = weigh[g * half : (g + 1) * half].T
        pieces = []
        for _ in range(3):
            piece = rest.astype(BF16).astype(F32)
            pieces.append(piece)
            rest = rest - piece
        spread[g] = jnp.concatenate(pieces, axis=1).astype(BF16)

    for i in range(2, 6):
        loads[i].wait()
    ext[pl.ds(RIM, length)] = input_gate[...].astype(F32) * conv_input[...].astype(F32)

    def gate_rows(lane):
        convolved = jnp.zeros((tokens, channels), F32)
        for j in range(tap_count):
            convolved = convolved + taps[j : j + 1, :].astype(F32) * ext[
                pl.ds(RIM - tap_count + 1 + j + lane * tokens, tokens)
            ]
        opened = output_gate[pl.ds(lane * tokens, tokens)].astype(F32)
        return (opened * convolved).astype(BF16)

    late = gate_rows(1)
    loads[6].wait()
    proj[1] = dot(late, out_proj[...])

    pl.semaphore_wait(barrier, peers)

    def rim_copy(which, target):
        src = (conv_input, input_gate)[which]
        return pltpu.make_async_remote_copy(
            src_ref=src.at[pl.ds(length - RIM, RIM)],
            dst_ref=rim.at[which],
            send_sem=rim_send.at[which],
            recv_sem=rim_recv.at[which],
            device_id=(target, core),
            device_id_type=MESH,
        )

    @pl.when(me < peers - 1)
    def _():
        for which in range(2):
            rim_copy(which, me + 1).start()

    proj_copy = pltpu.make_async_remote_copy(
        src_ref=proj.at[other],
        dst_ref=proj_in,
        send_sem=proj_send,
        recv_sem=proj_recv,
        device_id=(me, other),
        device_id_type=MESH,
    )

    @pl.when(core == 0)
    def _():
        proj_copy.start()

    @pl.when(me == 0)
    def _():
        ext[pl.ds(0, RIM)] = jnp.zeros((RIM, channels), F32)

    @pl.when(me > 0)
    def _():
        for which in range(2):
            rim_copy(which, me).wait_recv()
        ext[pl.ds(0, RIM)] = rim[1].astype(F32) * rim[0].astype(F32)

    proj[0] = dot(gate_rows(0), out_proj[...])

    @pl.when(core == 1)
    def _():
        proj_copy.start()

    loads[7].wait()
    loads[8].wait()
    proj_copy.wait_recv()
    stream = residual[...].astype(F32) + (proj[core] + proj_in[...])
    inverse_rms = lax.rsqrt(jnp.mean(stream * stream, axis=-1, keepdims=True) + 1e-06)
    normed = (stream * inverse_rms * gain[...]).astype(BF16)
    raw[...] = normed

    span_rows = per_group * rows
    if groups == 4:
        near = mine // 2 * 2
        far = lax.rem(near + 2, 4)
        side = mine - near
        beside, across, mirror = near + 1 - side, far + side, far + 1 - side
        middle = lax.rem(mine // 2 + side, 2)
        turn = middle * (beside - across)
        order = [mine, mirror, across + turn, beside - turn]
        sends = [mine, beside]
        distant = [mirror, across]
        partner = me + middle * (mirror - mine) * per_group
        anchor = me + (across - mine) * per_group
        shared = across + (1 - middle) * (mirror - across)
        hub = (mine + (1 - middle) * (beside - mine)) * per_group
    else:
        order = sends = [lax.rem(mine + step, groups) for step in range(groups)]
        distant = []
        middle, partner = 0, me
    column_half = width // 2

    def raw_copy(part_of):
        cols = pl.ds(part_of * column_half, column_half)
        return pltpu.make_async_remote_copy(
            src_ref=raw.at[:, cols],
            dst_ref=raw_in.at[:, cols],
            send_sem=raw_send.at[part_of],
            recv_sem=raw_recv.at[part_of],
            device_id=(partner, core),
            device_id_type=MESH,
        )

    def chosen_copy():
        return pltpu.make_async_remote_copy(
            src_ref=chosen.at[pl.ds(pl.multiple_of(far * span_rows, span_rows), 2 * span_rows)],
            dst_ref=chosen_in,
            send_sem=chosen_send,
            recv_sem=chosen_recv,
            device_id=(partner, core),
            device_id_type=MESH,
        )

    def spread_copy():
        return pltpu.make_async_remote_copy(
            src_ref=spread.at[pl.ds(far, 2)],
            dst_ref=spread_in,
            send_sem=spread_send,
            recv_sem=spread_recv,
            device_id=(anchor, core),
            device_id_type=MESH,
        )

    def sum_copy(part_of):
        cols = pl.ds(part_of * column_half, column_half)
        return pltpu.make_async_remote_copy(
            src_ref=summed.at[:, cols],
            dst_ref=sum_in.at[:, cols],
            send_sem=sum_send.at[part_of],
            recv_sem=sum_recv.at[part_of],
            device_id=(anchor, core),
            device_id_type=MESH,
        )

    if groups == 4:

        @pl.when(middle == 1)
        def _():
            chosen_copy().start()
            for part_of in range(2):
                raw_copy(part_of).start()

    def out_copy(slot, src, target):
        return pltpu.make_async_remote_copy(
            src_ref=outgoing.at[slot],
            dst_ref=recv.at[core, src],
            send_sem=out_send.at[slot],
            recv_sem=out_recv.at[src],
            device_id=(target, core),
            device_id_type=MESH,
        )

    def send_plane(plane):
        picked = chosen[pl.ds(pl.multiple_of(plane * span_rows, span_rows), span_rows)]
        slots = dot(picked, normed).astype(BF16).reshape(per_group, rows, width)
        outgoing[pl.ds(plane * per_group, per_group)] = slots

        @pl.loop(0, per_group)
        def _(i):
            target = plane * per_group + lax.rem(me + i, per_group)

            @pl.when(target != me)
            def _():
                out_copy(target, me, target).start()

    for plane in sends:
        send_plane(plane)
    recv[core, me] = outgoing[me]
    if groups == 4:

        @pl.when(middle == 0)
        def _():
            for plane in distant:
                send_plane(plane)
            spread_copy().start()

    proj_copy.wait_send()
    proj[core] = stream

    def gather_copy(src, slot, target, part_of):
        cols = pl.ds(part_of * column_half, column_half)
        return pltpu.make_async_remote_copy(
            src_ref=part.at[core, src, :, cols],
            dst_ref=gather.at[slot, :, cols],
            send_sem=ret_send.at[src],
            recv_sem=gather_recv.at[part_of, slot],
            device_id=(target, core),
            device_id_type=MESH,
        )

    def ret_part(src, part_of):
        cols = pl.ds(part_of * column_half, column_half)
        return pltpu.make_async_remote_copy(
            src_ref=part.at[core, src, :, cols],
            dst_ref=ret.at[me, :, cols],
            send_sem=ret_send.at[src],
            recv_sem=ret_recv.at[me],
            device_id=(src, core),
            device_id_type=MESH,
        )

    def fwd_copy(src, lane):
        return pltpu.make_async_remote_copy(
            src_ref=recv.at[lane, src],
            dst_ref=recv.at[lane, src],
            send_sem=fwd_send.at[src],
            recv_sem=fwd_recv.at[src],
            device_id=(me, other),
            device_id_type=MESH,
        )

    def ret_copy(src, slot, target):
        return pltpu.make_async_remote_copy(
            src_ref=part.at[core, src],
            dst_ref=ret.at[slot],
            send_sem=ret_send.at[src],
            recv_sem=ret_recv.at[slot],
            device_id=(target, core),
            device_id_type=MESH,
        )

    in_tile = tile_of(hidden, IN_TILE)
    out_tile = tile_of(width // 2, OUT_TILE)
    count = per_group
    lot = count * rows

    def begin(step):
        first = order[step] * per_group

        @pl.loop(0, count)
        def _(i):
            src = first + lax.rem(me + i, count)

            @pl.when((src != me) & (src != partner))
            def _():
                out_copy(src, src, src).wait_recv()

            fwd_copy(src, core).start()

    def relay():
        chosen_copy().wait_recv()
        for part_of in range(2):
            raw_copy(part_of).wait_recv()
            cols = pl.ds(part_of * column_half, column_half)
            picked = dot(chosen_in[...], raw_in[:, cols]).astype(BF16)
            outgoing[pl.ds(far * per_group, 2 * per_group), :, cols] = picked.reshape(
                2 * per_group, rows, column_half
            )

            @pl.loop(0, 2 * per_group)
            def _(i):
                target = near * per_group + lax.rem(me + i, 2 * per_group)
                slot = lax.rem(target + peers // 2, peers)

                @pl.when(target != me)
                def _():
                    pltpu.make_async_remote_copy(
                        src_ref=outgoing.at[slot, :, cols],
                        dst_ref=recv.at[core, partner, :, cols],
                        send_sem=out_send.at[slot],
                        recv_sem=out_recv.at[partner],
                        device_id=(target, core),
                        device_id_type=MESH,
                    ).start()

        recv[core, partner] = outgoing[lax.rem(me + peers // 2, peers)]

    def part_copy(step, side_of):
        span = pl.ds(order[step] * per_group, count)
        part_half = pl.ds(side_of * column_half, column_half)
        return pltpu.make_async_remote_copy(
            src_ref=part.at[other, span, :, part_half],
            dst_ref=part_in.at[step % 2, :, :, part_half],
            send_sem=part_send.at[step, side_of],
            recv_sem=part_recv.at[step, side_of],
            device_id=(me, other),
            device_id_type=MESH,
        )

    def raise_up(step):
        first = order[step] * per_group
        span = pl.ds(first, count)

        @pl.loop(0, count)
        def _(i):
            fwd_copy(first + lax.rem(me + i, count), other).wait_recv()

        @pl.loop(0, hidden // in_tile)
        def _(n):
            cols = pl.ds(pl.multiple_of(n * in_tile, in_tile), in_tile)
            x = recv[:, span].reshape(2 * lot, width)
            g = dot(x, gate[:, cols])
            u = dot(x, up[:, cols])
            active[:, cols] = (g * (1.0 / (1.0 + jnp.exp(-g))) * u).astype(BF16)

    def bring_down(step):
        span = pl.ds(order[step] * per_group, count)
        for side_of in range(2):
            start = side_of * column_half

            @pl.loop(0, column_half // out_tile)
            def _(n):
                cols = pl.ds(pl.multiple_of(start + n * out_tile, 128), out_tile)
                y = dot(active[...], down[:, cols]).astype(BF16)
                part[:, span, :, cols] = y.reshape(2, count, rows, out_tile)

            part_copy(step, side_of).start()

    def tail(step):
        first = order[step] * per_group
        for part_of in range(2):
            part_copy(step, part_of).wait()
            cols = pl.ds(part_of * column_half, column_half)

            @pl.loop(0, count)
            def _(i):
                place = lax.rem(me + i, count)
                src = first + place
                theirs = part_in[step % 2, place, :, cols].astype(F32)
                mixed = part[core, src, :, cols].astype(F32) + theirs
                halves = mixed.astype(BF16)
                part[core, src, :, cols] = halves
                if groups == 4:
                    target = hub + lax.rem(src, per_group)
                    slot = lax.rem(me, 2 * per_group)

                    @pl.when((order[step] != shared) & (src != me))
                    def _():
                        ret_part(src, part_of).start()

                    @pl.when((order[step] == shared) & (target != me))
                    def _():
                        gather_copy(src, slot, target, part_of).start()

                    @pl.when((order[step] == shared) & (target == me))
                    def _():
                        gather[slot, :, cols] = halves

                else:

                    @pl.when(src != me)
                    def _():
                        ret_part(src, part_of).start()

                @pl.when(src == me)
                def _():
                    ret[me, :, cols] = halves

    def share():
        spread_copy().wait_recv()
        for part_of in range(2):

            @pl.loop(0, 2 * per_group)
            def _(i):
                @pl.when(near * per_group + i != me)
                def _():
                    gather_copy(me, i, me, part_of).wait_recv()

            for n in range(column_half // out_tile):
                cols = pl.ds(part_of * column_half + n * out_tile, out_tile)
                added = jnp.zeros((tokens, out_tile), F32)
                for j in range(2):
                    values = gather[pl.ds(j * per_group, per_group), :, cols]
                    values = values.reshape(lot, out_tile)
                    added = added + dot(spread_in[j], jnp.concatenate([values] * 3, axis=0))
                summed[:, cols] = added.astype(BF16)
            sum_copy(part_of).start()

    if groups == 4:

        @pl.when(middle == 1)
        def _():
            relay()

    begin(0)
    for step in range(groups):
        if step == 0:
            loads[9].wait()
            loads[10].wait()
        raise_up(step)
        if step == 0:
            loads[11].wait()
        if step == 2:

            @pl.when(middle == 1)
            def _():
                tail(1)

        elif step > 0:
            tail(step - 1)
        if step < groups - 1:
            begin(step + 1)
        bring_down(step)
        if groups == 4 and step == 1:

            @pl.when(middle == 0)
            def _():
                tail(1)

    tail(groups - 1)

    if groups == 4:

        @pl.when(middle == 1)
        def _():
            share()

    def store(part_of):
        cols = pl.ds(part_of * column_half, column_half)
        return pltpu.make_async_copy(out.at[:, cols], out_hbm.at[:, cols], out_copy_sem.at[part_of])

    def add_plane(plane, last):
        first = plane * per_group

        @pl.loop(0, count)
        def _(i):
            src = first + i

            @pl.when(src != me)
            def _():
                ret_copy(src, src, src).wait_recv()

        for n in range(width // out_tile):
            cols = pl.ds(n * out_tile, out_tile)
            part_of = (n + 1) * out_tile // column_half - 1
            whole = (n + 1) * out_tile % column_half == 0
            values = ret[pl.ds(first, count), :, cols].reshape(lot, out_tile)
            added = proj[core, :, cols] + dot(
                spread[plane], jnp.concatenate([values] * 3, axis=0)
            )
            if last:
                out[:, cols] = added.astype(BF16)
                if whole:
                    store(part_of).start()
            else:
                proj[core, :, cols] = added

    for step, plane in enumerate(sends):
        add_plane(plane, groups != 4 and step == groups - 1)
    if groups == 4:

        @pl.when(middle == 1)
        def _():
            add_plane(mirror, False)
            add_plane(across, True)

        @pl.when(middle == 0)
        def _():
            for part_of in range(2):
                cols = pl.ds(part_of * column_half, column_half)
                sum_copy(part_of).wait_recv()
                out[:, cols] = (proj[core, :, cols] + sum_in[:, cols].astype(F32)).astype(BF16)
                store(part_of).start()

    @pl.loop(0, peers)
    def _(src):
        @pl.when((src != me) & (lax.rem(src + middle * (peers // 2), peers) != me))
        def _():
            out_copy(src, src, src).wait_send()

        held = anchor if groups == 4 else me

        @pl.when((src != me) & ((middle == 0) | (src != held)))
        def _():
            ret_copy(src, src, src).wait_send()

        fwd_copy(src, core).wait_send()

    if groups == 4:

        @pl.when(middle == 1)
        def _():
            chosen_copy().wait_send()
            for part_of in range(2):
                raw_copy(part_of).wait_send()
                sum_copy(part_of).wait_send()

        @pl.when(middle == 0)
        def _():
            spread_copy().wait_send()

    @pl.when(me < peers - 1)
    def _():
        for which in range(2):
            rim_copy(which, me + 1).wait_send()

    for part_of in range(2):
        store(part_of).wait()


def per_device(
    residual,
    conv_input,
    input_gate,
    output_gate,
    conv_taps,
    out_proj,
    norm_gain,
    routes,
    route_weight,
    gate_proj,
    up_proj,
    down_proj,
):
    peers = lax.axis_size("sp")
    tokens, width = residual.shape
    length, channels = conv_input.shape
    hidden = gate_proj.shape[2]
    capacity = 2 * tokens * routes.shape[1] // peers
    rows = -(-capacity // 16) * 16
    groups = 4 if peers % 4 == 0 else 1
    half = peers // groups * rows
    relayed = 2 * half if groups == 4 else rows
    grant = 67043328
    dma = pltpu.SemaphoreType.DMA
    hbm = pl.BlockSpec(memory_space=pltpu.HBM)
    return pl.pallas_call(
        functools.partial(kernel, peers, groups, rows),
        out_shape=jax.ShapeDtypeStruct((tokens, width), BF16),
        in_specs=[hbm] * 12,
        out_specs=hbm,
        scratch_shapes=[
            pltpu.VMEM((tokens, width), BF16),
            pltpu.VMEM(residual.shape, BF16),
            pltpu.VMEM(conv_input.shape, BF16),
            pltpu.VMEM(input_gate.shape, BF16),
            pltpu.VMEM(output_gate.shape, BF16),
            pltpu.VMEM(conv_taps.shape, BF16),
            pltpu.VMEM((1, width), F32),
            pltpu.VMEM(routes.shape[::-1], jnp.int32),
            pltpu.VMEM(route_weight.shape[::-1], F32),
            pltpu.VMEM(out_proj.shape, BF16),
            pltpu.VMEM(gate_proj.shape[1:], BF16),
            pltpu.VMEM(up_proj.shape[1:], BF16),
            pltpu.VMEM(down_proj.shape[1:], BF16),
            pltpu.VMEM((2, RIM, channels), BF16),
            pltpu.VMEM((RIM + length, channels), F32),
            pltpu.VMEM((peers * rows, tokens), BF16),
            pltpu.VMEM((2, tokens, width), F32),
            pltpu.VMEM((tokens, width), F32),
            pltpu.VMEM((tokens, width), BF16),
            pltpu.VMEM((tokens, width), BF16),
            pltpu.VMEM((relayed, tokens), BF16),
            pltpu.VMEM((peers, rows, width), BF16),
            pltpu.VMEM((2, peers, rows, width), BF16),
            pltpu.VMEM((2 * half, hidden), BF16),
            pltpu.VMEM((2, peers, rows, width), BF16),
            pltpu.VMEM((2, peers // groups, rows, width), BF16),
            pltpu.VMEM((peers, rows, width), BF16),
            pltpu.VMEM((groups, tokens, 3 * half), BF16),
            pltpu.VMEM((2, tokens, 3 * half), BF16),
            pltpu.VMEM((peers // 2, rows, width), BF16),
            pltpu.VMEM((tokens, width), BF16),
            pltpu.VMEM((tokens, width), BF16),
            dma((2,)),
            dma((12,)),
            dma((2,)),
            dma((2,)),
            dma,
            dma,
            dma((2,)),
            dma((2,)),
            dma,
            dma,
            dma((peers,)),
            dma((peers,)),
            dma((peers,)),
            dma((peers,)),
            dma((groups, 2)),
            dma((groups, 2)),
            dma((peers,)),
            dma((peers,)),
            dma,
            dma,
            dma((2, peers // 2)),
            dma((2,)),
            dma((2,)),
        ],
        compiler_params=pltpu.CompilerParams(
            collective_id=0, has_side_effects=True, vmem_limit_bytes=grant
        ),
        name="mixer_experts",
    )(
        residual,
        conv_input,
        input_gate,
        output_gate,
        conv_taps,
        norm_gain.reshape(1, width),
        routes.T,
        route_weight.T,
        out_proj,
        gate_proj,
        up_proj,
        down_proj,
    )


def solution(mesh):
    return jax.shard_map(
        per_device,
        mesh=mesh,
        in_specs=(
            P(("sp", "tp"), None),
            P("sp", "tp"),
            P("sp", "tp"),
            P("sp", "tp"),
            P(None, "tp"),
            P("tp", None),
            P(),
            P(("sp", "tp"), None),
            P(("sp", "tp"), None),
            P("sp", None, "tp"),
            P("sp", None, "tp"),
            P("sp", "tp", None),
        ),
        out_specs=P(("sp", "tp"), None),
        check_vma=False,
    )
```

```python
import functools

import jax
import jax.numpy as jnp
from jax import lax
from jax.experimental import pallas as pl
from jax.experimental.pallas import tpu as pltpu
from jax.sharding import PartitionSpec as P

MESH = pl.DeviceIdType.MESH
F32 = jnp.float32
BF16 = jnp.bfloat16
RIM = 16


OUT_TILE = 1024


def tile_of(size, most):
    for tile in range(most, 127, -128):
        if size % tile == 0:
            return tile
    return size


def dot(a, b):
    return jnp.dot(a, b, preferred_element_type=F32)


def kernel(
    peers,
    groups,
    rows,
    residual_hbm,
    conv_input_hbm,
    input_gate_hbm,
    output_gate_hbm,
    taps_hbm,
    gain_hbm,
    routes_hbm,
    weights_hbm,
    out_proj_hbm,
    gate_hbm,
    up_hbm,
    down_hbm,
    out_hbm,
    out,
    residual,
    conv_input,
    input_gate,
    output_gate,
    taps,
    gain,
    routes,
    weights,
    out_proj,
    gate,
    up,
    down,
    rim,
    ext,
    chosen,
    proj,
    proj_in,
    raw,
    raw_in,
    chosen_in,
    outgoing,
    recv,
    active,
    part,
    part_in,
    ret,
    spread,
    spread_in,
    gather,
    summed,
    sum_in,
    out_copy_sem,
    load_sem,
    rim_send,
    rim_recv,
    proj_send,
    proj_recv,
    raw_send,
    raw_recv,
    chosen_send,
    chosen_recv,
    out_send,
    out_recv,
    fwd_send,
    fwd_recv,
    part_send,
    part_recv,
    ret_send,
    ret_recv,
    spread_send,
    spread_recv,
    gather_recv,
    sum_send,
    sum_recv,
):
    me = lax.axis_index("sp")
    core = lax.axis_index("tp")
    other = 1 - core
    length, channels = conv_input.shape
    tokens, width = residual.shape
    hidden = gate.shape[1]
    tap_count = taps.shape[0]
    per_group = peers // groups

    barrier = pltpu.get_barrier_semaphore()


    @pl.loop(1, peers)
    def _(k):
        pl.semaphore_signal(
            barrier, inc=1, device_id=(lax.rem(me + k, peers), core), device_id_type=MESH
        )

    pl.semaphore_signal(barrier, inc=1, device_id=(me, other), device_id_type=MESH)
    mine = me // per_group

    loads = []
    for i, (src, dst) in enumerate(
        (
            (routes_hbm, routes),
            (weights_hbm, weights),
            (conv_input_hbm, conv_input),
            (input_gate_hbm, input_gate),
            (output_gate_hbm, output_gate),
            (taps_hbm, taps),
            (out_proj_hbm, out_proj),
            (residual_hbm, residual),
            (gain_hbm, gain),
            (gate_hbm.at[0], gate),
            (up_hbm.at[0], up),
            (down_hbm.at[0], down),
        )
    ):
        load = pltpu.make_async_copy(src, dst, load_sem.at[i])
        load.start()
        loads.append(load)

    loads[0].wait()
    loads[1].wait()
    tops = routes.shape[0]
    ids = lax.broadcasted_iota(jnp.int32, (peers, tokens), 0)
    hots = [(routes[k : k + 1, :] == ids).astype(F32) for k in range(tops)]
    total = functools.reduce(jnp.add, hots)
    earlier = (
        lax.broadcasted_iota(jnp.int32, (tokens, tokens), 0)
        < lax.broadcasted_iota(jnp.int32, (tokens, tokens), 1)
    ).astype(BF16)
    counts = dot(total.astype(BF16), earlier)
    lines = lax.broadcasted_iota(jnp.int32, (peers * rows, tokens), 0)
    select = jnp.zeros((peers * rows, tokens), F32)
    weigh = jnp.zeros((peers * rows, tokens), F32)
    for k in range(tops):
        slot = jnp.sum(counts * hots[k], axis=0, keepdims=True).astype(jnp.int32)
        hit = lines == routes[k : k + 1, :] * rows + slot
        select = jnp.where(hit, 1.0, select)
        weigh = jnp.where(hit, weights[k : k + 1, :], weigh)
    chosen[...] = select.astype(BF16)
    half = per_group * rows
    for g in range(groups):
        rest = weigh[g * half : (g + 1) * half].T
        pieces = []
        for _ in range(3):
            piece = rest.astype(BF16).astype(F32)
            pieces.append(piece)
            rest = rest - piece
        spread[g] = jnp.concatenate(pieces, axis=1).astype(BF16)

    for i in range(2, 6):
        loads[i].wait()
    ext[pl.ds(RIM, length)] = input_gate[...].astype(F32) * conv_input[...].astype(F32)

    def gate_rows(lane):
        convolved = jnp.zeros((tokens, channels), F32)
        for j in range(tap_count):
            convolved = convolved + taps[j : j + 1, :].astype(F32) * ext[
                pl.ds(RIM - tap_count + 1 + j + lane * tokens, tokens)
            ]
        opened = output_gate[pl.ds(lane * tokens, tokens)].astype(F32)
        return (opened * convolved).astype(BF16)

    late = gate_rows(1)
    loads[6].wait()
    proj[1] = dot(late, out_proj[...])

    pl.semaphore_wait(barrier, peers)

    def rim_copy(which, target):
        src = (conv_input, input_gate)[which]
        return pltpu.make_async_remote_copy(
            src_ref=src.at[pl.ds(length - RIM, RIM)],
            dst_ref=rim.at[which],
            send_sem=rim_send.at[which],
            recv_sem=rim_recv.at[which],
            device_id=(target, core),
            device_id_type=MESH,
        )

    @pl.when(me < peers - 1)
    def _():
        for which in range(2):
            rim_copy(which, me + 1).start()

    proj_copy = pltpu.make_async_remote_copy(
        src_ref=proj.at[other],
        dst_ref=proj_in,
        send_sem=proj_send,
        recv_sem=proj_recv,
        device_id=(me, other),
        device_id_type=MESH,
    )

    @pl.when(core == 0)
    def _():
        proj_copy.start()

    def early_rows():
        @pl.when(me == 0)
        def _():
            ext[pl.ds(0, RIM)] = jnp.zeros((RIM, channels), F32)

        @pl.when(me > 0)
        def _():
            for which in range(2):
                rim_copy(which, me).wait_recv()
            ext[pl.ds(0, RIM)] = rim[1].astype(F32) * rim[0].astype(F32)

        proj[0] = dot(gate_rows(0), out_proj[...])

    pl.when(core == 0)(early_rows)
    loads[7].wait()
    loads[8].wait()
    proj_copy.wait_recv()
    stream = residual[...].astype(F32) + (proj[core] + proj_in[...])
    inverse_rms = lax.rsqrt(jnp.mean(stream * stream, axis=-1, keepdims=True) + 1e-06)
    normed = (stream * inverse_rms * gain[...]).astype(BF16)
    raw[...] = normed

    span_rows = per_group * rows
    if groups == 4:
        near = mine // 2 * 2
        far = lax.rem(near + 2, 4)
        side = mine - near
        beside, across, mirror = near + 1 - side, far + side, far + 1 - side
        middle = lax.rem(mine // 2 + side, 2)
        turn = middle * (beside - across)
        order = [mine, mirror, across + turn, beside - turn]
        sends = [mine, beside]
        distant = [mirror, across]
        partner = me + middle * (mirror - mine) * per_group
        anchor = me + (across - mine) * per_group
        shared = across + (1 - middle) * (mirror - across)
        hub = (mine + (1 - middle) * (beside - mine)) * per_group
    else:
        order = sends = [lax.rem(mine + step, groups) for step in range(groups)]
        distant = []
        middle, partner = 0, me
    column_half = width // 2

    def raw_copy(part_of):
        cols = pl.ds(part_of * column_half, column_half)
        return pltpu.make_async_remote_copy(
            src_ref=raw.at[:, cols],
            dst_ref=raw_in.at[:, cols],
            send_sem=raw_send.at[part_of],
            recv_sem=raw_recv.at[part_of],
            device_id=(partner, core),
            device_id_type=MESH,
        )

    def chosen_copy():
        return pltpu.make_async_remote_copy(
            src_ref=chosen.at[pl.ds(pl.multiple_of(far * span_rows, span_rows), 2 * span_rows)],
            dst_ref=chosen_in,
            send_sem=chosen_send,
            recv_sem=chosen_recv,
            device_id=(partner, core),
            device_id_type=MESH,
        )

    def spread_copy():
        return pltpu.make_async_remote_copy(
            src_ref=spread.at[pl.ds(far, 2)],
            dst_ref=spread_in,
            send_sem=spread_send,
            recv_sem=spread_recv,
            device_id=(anchor, core),
            device_id_type=MESH,
        )

    def sum_copy(part_of):
        cols = pl.ds(part_of * column_half, column_half)
        return pltpu.make_async_remote_copy(
            src_ref=summed.at[:, cols],
            dst_ref=sum_in.at[:, cols],
            send_sem=sum_send.at[part_of],
            recv_sem=sum_recv.at[part_of],
            device_id=(anchor, core),
            device_id_type=MESH,
        )

    if groups == 4:

        @pl.when(middle == 1)
        def _():
            chosen_copy().start()
            for part_of in range(2):
                raw_copy(part_of).start()

    def out_copy(slot, src, target):
        return pltpu.make_async_remote_copy(
            src_ref=outgoing.at[slot],
            dst_ref=recv.at[core, src],
            send_sem=out_send.at[slot],
            recv_sem=out_recv.at[src],
            device_id=(target, core),
            device_id_type=MESH,
        )

    def send_plane(plane):
        picked = chosen[pl.ds(pl.multiple_of(plane * span_rows, span_rows), span_rows)]
        slots = dot(picked, raw[...]).astype(BF16).reshape(per_group, rows, width)
        outgoing[pl.ds(plane * per_group, per_group)] = slots

        @pl.loop(0, per_group)
        def _(i):
            target = plane * per_group + lax.rem(me + i, per_group)

            @pl.when(target != me)
            def _():
                out_copy(target, me, target).start()

    for plane in sends:
        send_plane(plane)
    recv[core, me] = outgoing[me]
    proj[core] = stream

    def send_far():
        for plane in distant:
            send_plane(plane)
        spread_copy().start()

    if groups == 4:
        pl.when((middle == 0) & (core == 0))(send_far)


    @pl.when(core == 1)
    def _():
        early_rows()
        proj_copy.start()

    proj_copy.wait_send()

    def gather_copy(src, slot, target, part_of):
        cols = pl.ds(part_of * column_half, column_half)
        return pltpu.make_async_remote_copy(
            src_ref=part.at[core, src, :, cols],
            dst_ref=gather.at[slot, :, cols],
            send_sem=ret_send.at[src],
            recv_sem=gather_recv.at[part_of, slot],
            device_id=(target, core),
            device_id_type=MESH,
        )

    def ret_part(src, part_of):
        cols = pl.ds(part_of * column_half, column_half)
        return pltpu.make_async_remote_copy(
            src_ref=part.at[core, src, :, cols],
            dst_ref=ret.at[me, :, cols],
            send_sem=ret_send.at[src],
            recv_sem=ret_recv.at[me],
            device_id=(src, core),
            device_id_type=MESH,
        )

    def fwd_copy(src, lane):
        return pltpu.make_async_remote_copy(
            src_ref=recv.at[lane, src],
            dst_ref=recv.at[lane, src],
            send_sem=fwd_send.at[src],
            recv_sem=fwd_recv.at[src],
            device_id=(me, other),
            device_id_type=MESH,
        )

    def ret_copy(src, slot, target):
        return pltpu.make_async_remote_copy(
            src_ref=part.at[core, src],
            dst_ref=ret.at[slot],
            send_sem=ret_send.at[src],
            recv_sem=ret_recv.at[slot],
            device_id=(target, core),
            device_id_type=MESH,
        )

    cut = -(-hidden // 512) * 256
    out_tile = tile_of(width // 2, OUT_TILE)
    count = per_group
    lot = count * rows

    def begin(step):
        first = order[step] * per_group

        @pl.loop(0, count)
        def _(i):
            src = first + lax.rem(me + i, count)

            @pl.when((src != me) & (src != partner))
            def _():
                out_copy(src, src, src).wait_recv()

            fwd_copy(src, core).start()

    def relay():
        chosen_copy().wait_recv()
        for part_of in range(2):
            raw_copy(part_of).wait_recv()
            cols = pl.ds(part_of * column_half, column_half)
            picked = dot(chosen_in[...], raw_in[:, cols]).astype(BF16)
            outgoing[pl.ds(far * per_group, 2 * per_group), :, cols] = picked.reshape(
                2 * per_group, rows, column_half
            )

            @pl.loop(0, 2 * per_group)
            def _(i):
                target = near * per_group + lax.rem(me + i, 2 * per_group)
                slot = lax.rem(target + peers // 2, peers)

                @pl.when(target != me)
                def _():
                    pltpu.make_async_remote_copy(
                        src_ref=outgoing.at[slot, :, cols],
                        dst_ref=recv.at[core, partner, :, cols],
                        send_sem=out_send.at[slot],
                        recv_sem=out_recv.at[partner],
                        device_id=(target, core),
                        device_id_type=MESH,
                    ).start()

        recv[core, partner] = outgoing[lax.rem(me + peers // 2, peers)]

    def part_copy(step, side_of):
        span = pl.ds(order[step] * per_group, count)
        part_half = pl.ds(side_of * column_half, column_half)
        return pltpu.make_async_remote_copy(
            src_ref=part.at[other, span, :, part_half],
            dst_ref=part_in.at[step % 2, :, :, part_half],
            send_sem=part_send.at[step, side_of],
            recv_sem=part_recv.at[step, side_of],
            device_id=(me, other),
            device_id_type=MESH,
        )

    def raise_up(step, between):
        first = order[step] * per_group
        span = pl.ds(first, count)

        @pl.loop(0, count)
        def _(i):
            fwd_copy(first + lax.rem(me + i, count), other).wait_recv()

        for start, size in ((0, cut), (cut, hidden - cut)):
            if start:
                between()
            cols = pl.ds(start, size)
            x = recv[:, span].reshape(2 * lot, width)
            g = dot(x, gate[:, cols])
            u = dot(x, up[:, cols])
            active[:, cols] = (g * (1.0 / (1.0 + jnp.exp(-g))) * u).astype(BF16)

    def bring_down(step):
        span = pl.ds(order[step] * per_group, count)
        for side_of in range(2):
            start = side_of * column_half

            @pl.loop(0, column_half // out_tile)
            def _(n):
                cols = pl.ds(pl.multiple_of(start + n * out_tile, 128), out_tile)
                y = dot(active[...], down[:, cols]).astype(BF16)
                part[:, span, :, cols] = y.reshape(2, count, rows, out_tile)

            part_copy(step, side_of).start()

    def tail(step):
        first = order[step] * per_group
        for part_of in range(2):
            part_copy(step, part_of).wait()
            cols = pl.ds(part_of * column_half, column_half)

            @pl.loop(0, count)
            def _(i):
                place = lax.rem(me + i, count)
                src = first + place
                theirs = part_in[step % 2, place, :, cols].astype(F32)
                mixed = part[core, src, :, cols].astype(F32) + theirs
                halves = mixed.astype(BF16)
                part[core, src, :, cols] = halves
                if groups == 4:
                    target = hub + lax.rem(src, per_group)
                    slot = lax.rem(me, 2 * per_group)

                    @pl.when((order[step] != shared) & (src != me))
                    def _():
                        ret_part(src, part_of).start()

                    @pl.when((order[step] == shared) & (target != me))
                    def _():
                        gather_copy(src, slot, target, part_of).start()

                    @pl.when((order[step] == shared) & (target == me))
                    def _():
                        gather[slot, :, cols] = halves

                else:

                    @pl.when(src != me)
                    def _():
                        ret_part(src, part_of).start()

                @pl.when(src == me)
                def _():
                    ret[me, :, cols] = halves

    def share():
        spread_copy().wait_recv()
        for part_of in range(2):

            @pl.loop(0, 2 * per_group)
            def _(i):
                @pl.when(near * per_group + i != me)
                def _():
                    gather_copy(me, i, me, part_of).wait_recv()

            for n in range(column_half // out_tile):
                cols = pl.ds(part_of * column_half + n * out_tile, out_tile)
                added = jnp.zeros((tokens, out_tile), F32)
                for j in range(2):
                    values = gather[pl.ds(j * per_group, per_group), :, cols]
                    values = values.reshape(lot, out_tile)
                    added = added + dot(spread_in[j], jnp.concatenate([values] * 3, axis=0))
                summed[:, cols] = added.astype(BF16)
            sum_copy(part_of).start()

    if groups == 4:

        @pl.when(middle == 1)
        def _():
            relay()

    begin(0)
    if groups == 4:
        pl.when((middle == 0) & (core == 1))(send_far)

    for step in range(groups):
        if step == 0:
            loads[9].wait()
            loads[10].wait()
        raise_up(step, functools.partial(tail, step - 1) if step > 0 else loads[11].wait)
        if step < groups - 1:
            begin(step + 1)
        bring_down(step)
    tail(groups - 1)

    if groups == 4:

        @pl.when(middle == 1)
        def _():
            share()

    def store(part_of):
        cols = pl.ds(part_of * column_half, column_half)
        return pltpu.make_async_copy(out.at[:, cols], out_hbm.at[:, cols], out_copy_sem.at[part_of])

    def add_plane(plane, last):
        first = plane * per_group

        @pl.loop(0, count)
        def _(i):
            src = first + i

            @pl.when(src != me)
            def _():
                ret_copy(src, src, src).wait_recv()

        for n in range(width // out_tile):
            cols = pl.ds(n * out_tile, out_tile)
            part_of = (n + 1) * out_tile // column_half - 1
            whole = (n + 1) * out_tile % column_half == 0
            values = ret[pl.ds(first, count), :, cols].reshape(lot, out_tile)
            added = proj[core, :, cols] + dot(
                spread[plane], jnp.concatenate([values] * 3, axis=0)
            )
            if last:
                out[:, cols] = added.astype(BF16)
                if whole:
                    store(part_of).start()
            else:
                proj[core, :, cols] = added

    if groups == 4:
        add_plane(mine, False)

    @pl.loop(0, peers)
    def _(src):
        @pl.when((src != me) & (lax.rem(src + middle * (peers // 2), peers) != me))
        def _():
            out_copy(src, src, src).wait_send()

        held = anchor if groups == 4 else me

        @pl.when((src != me) & ((middle == 0) | (src != held)))
        def _():
            ret_copy(src, src, src).wait_send()

        fwd_copy(src, core).wait_send()

    if groups == 4:

        @pl.when(middle == 1)
        def _():
            chosen_copy().wait_send()
            for part_of in range(2):
                raw_copy(part_of).wait_send()
                sum_copy(part_of).wait_send()

        @pl.when(middle == 0)
        def _():
            spread_copy().wait_send()

    @pl.when(me < peers - 1)
    def _():
        for which in range(2):
            rim_copy(which, me + 1).wait_send()

    if groups == 4:

        @pl.when(middle == 1)
        def _():
            add_plane(mirror, False)
            add_plane(across, False)
            add_plane(beside, True)

        @pl.when(middle == 0)
        def _():
            add_plane(beside, False)
            for part_of in range(2):
                cols = pl.ds(part_of * column_half, column_half)
                sum_copy(part_of).wait_recv()
                out[:, cols] = (proj[core, :, cols] + sum_in[:, cols].astype(F32)).astype(BF16)
                store(part_of).start()

    else:
        for step, plane in enumerate(sends):
            add_plane(plane, step == groups - 1)

    for part_of in range(2):
        store(part_of).wait()


def per_device(
    residual,
    conv_input,
    input_gate,
    output_gate,
    conv_taps,
    out_proj,
    norm_gain,
    routes,
    route_weight,
    gate_proj,
    up_proj,
    down_proj,
):
    peers = lax.axis_size("sp")
    tokens, width = residual.shape
    length, channels = conv_input.shape
    hidden = gate_proj.shape[2]
    capacity = 2 * tokens * routes.shape[1] // peers
    rows = -(-capacity // 16) * 16
    groups = 4 if peers % 4 == 0 else 1
    half = peers // groups * rows
    relayed = 2 * half if groups == 4 else rows
    grant = 67043328
    dma = pltpu.SemaphoreType.DMA
    hbm = pl.BlockSpec(memory_space=pltpu.HBM)
    return pl.pallas_call(
        functools.partial(kernel, peers, groups, rows),
        out_shape=jax.ShapeDtypeStruct((tokens, width), BF16),
        in_specs=[hbm] * 12,
        out_specs=hbm,
        scratch_shapes=[
            pltpu.VMEM((tokens, width), BF16),
            pltpu.VMEM(residual.shape, BF16),
            pltpu.VMEM(conv_input.shape, BF16),
            pltpu.VMEM(input_gate.shape, BF16),
            pltpu.VMEM(output_gate.shape, BF16),
            pltpu.VMEM(conv_taps.shape, BF16),
            pltpu.VMEM((1, width), F32),
            pltpu.VMEM(routes.shape[::-1], jnp.int32),
            pltpu.VMEM(route_weight.shape[::-1], F32),
            pltpu.VMEM(out_proj.shape, BF16),
            pltpu.VMEM(gate_proj.shape[1:], BF16),
            pltpu.VMEM(up_proj.shape[1:], BF16),
            pltpu.VMEM(down_proj.shape[1:], BF16),
            pltpu.VMEM((2, RIM, channels), BF16),
            pltpu.VMEM((RIM + length, channels), F32),
            pltpu.VMEM((peers * rows, tokens), BF16),
            pltpu.VMEM((2, tokens, width), F32),
            pltpu.VMEM((tokens, width), F32),
            pltpu.VMEM((tokens, width), BF16),
            pltpu.VMEM((tokens, width), BF16),
            pltpu.VMEM((relayed, tokens), BF16),
            pltpu.VMEM((peers, rows, width), BF16),
            pltpu.VMEM((2, peers, rows, width), BF16),
            pltpu.VMEM((2 * half, hidden), BF16),
            pltpu.VMEM((2, peers, rows, width), BF16),
            pltpu.VMEM((2, peers // groups, rows, width), BF16),
            pltpu.VMEM((peers, rows, width), BF16),
            pltpu.VMEM((groups, tokens, 3 * half), BF16),
            pltpu.VMEM((2, tokens, 3 * half), BF16),
            pltpu.VMEM((peers // 2, rows, width), BF16),
            pltpu.VMEM((tokens, width), BF16),
            pltpu.VMEM((tokens, width), BF16),
            dma((2,)),
            dma((12,)),
            dma((2,)),
            dma((2,)),
            dma,
            dma,
            dma((2,)),
            dma((2,)),
            dma,
            dma,
            dma((peers,)),
            dma((peers,)),
            dma((peers,)),
            dma((peers,)),
            dma((groups, 2)),
            dma((groups, 2)),
            dma((peers,)),
            dma((peers,)),
            dma,
            dma,
            dma((2, peers // 2)),
            dma((2,)),
            dma((2,)),
        ],
        compiler_params=pltpu.CompilerParams(
            collective_id=0, has_side_effects=True, vmem_limit_bytes=grant
        ),
        name="mixer_experts",
    )(
        residual,
        conv_input,
        input_gate,
        output_gate,
        conv_taps,
        norm_gain.reshape(1, width),
        routes.T,
        route_weight.T,
        out_proj,
        gate_proj,
        up_proj,
        down_proj,
    )


def solution(mesh):
    return jax.shard_map(
        per_device,
        mesh=mesh,
        in_specs=(
            P(("sp", "tp"), None),
            P("sp", "tp"),
            P("sp", "tp"),
            P("sp", "tp"),
            P(None, "tp"),
            P("tp", None),
            P(),
            P(("sp", "tp"), None),
            P(("sp", "tp"), None),
            P("sp", None, "tp"),
            P("sp", None, "tp"),
            P("sp", "tp", None),
        ),
        out_specs=P(("sp", "tp"), None),
        check_vma=False,
    )
```
